512 devices in a mesh: sp: 32 (over z, core), tp: 16 (over y, x).
Axes of the slice: x: 4, y: 4, z: 16, core: 2. Of those that a mesh axis runs over, the one named last changes fastest.
Arguments:
- residual_input: bfloat16 [4096, 2048], P(('sp', 'tp')), may hold values from -6 to 6
- mixer_value_input: bfloat16 [4096, 2048], P('sp', 'tp'), may hold values from -6 to 6
- gate_preactivation: bfloat16 [4096, 2048], P('sp', 'tp'), may hold values from -6 to 6
- state_projection_input: bfloat16 [4096, 2, 4, 128], P('sp'), may hold values from -6 to 6
- step_preactivation: bfloat16 [4096, 2, 32], P('sp', None, 'tp'), may hold values from -6 to 6
- spike_log_decay: float32 [4096, 2, 32], P('sp', None, 'tp'), may hold values from -1 to 0
- value_filter_taps: float32 [5, 2048], P(None, 'tp'), may hold values from -2.5 to 2.5
- state_projection_taps: float32 [5, 2, 4, 128], replicated, may hold values from -2.5 to 2.5
- step_size_bias: float32 [2, 32], P(None, 'tp'), may hold values from -0.5 to 0.5
- head_log_decay: float32 [2, 32], P(None, 'tp'), may hold values from -12 to -3
- gated_norm_gain: float32 [2048], P('tp'), may hold values from 0.1 to 1.9
- mixer_output_weight: bfloat16 [2048, 2048], P('tp'), may hold values from -0.125 to 0.125
- feedforward_norm_gain: float32 [2048], replicated, may hold values from 0.1 to 1.9
- routed_expert_index: int32 [4096, 4], P('sp'), may hold values from 0 to 31, all different within a row; in each aligned block of 128 rows (0 to 127, 128 to 255, ...) at most 24 rows name the same one
- routed_expert_weight: float32 [4096, 4], P('sp'), may hold values from 0.2 to 1.2
- routed_gate_weight: bfloat16 [32, 2048, 2048], P('sp', None, 'tp'), may hold values from -0.125 to 0.125
- routed_up_weight: bfloat16 [32, 2048, 2048], P('sp', None, 'tp'), may hold values from -0.125 to 0.125
- routed_down_weight: bfloat16 [32, 2048, 2048], P('sp', 'tp'), may hold values from -0.1875 to 0.1875
- common_gate_weight: bfloat16 [2048, 2048], P(None, 'tp'), may hold values from -0.125 to 0.125
- common_up_weight: bfloat16 [2048, 2048], P(None, 'tp'), may hold values from -0.125 to 0.125
- common_down_weight: bfloat16 [2048, 2048], P('tp'), may hold values from -0.125 to 0.125
Outputs:
- layer_out: bfloat16 [4096, 2048], P(('sp', 'tp'))
The draws below stay inside these ranges and needn't reach their ends.
Inputs may be any that keep to these rules, and one draw needn't show every extreme that they name: `routed_expert_index`: each row names 4 different experts. In the aligned blocks of 128 rows no expert is named by more than 24 rows, and in some block one expert is named by exactly 24.
All inputs are finite; a program needn't handle non-finite values.
Results may differ from the reference program's by a relative error of at most 0.02.
Values may be sent and summed in bfloat16 or wider, within the bound.
A program may use at most 64 MiB of HBM per device.

```python
import math
import jax
import jax.numpy as jnp
import numpy as np
from jax import lax

D = 2048
HEADS = 32
HD = 64
GROUPS = 4
STATE = 128
CONV = 5
BLK = 128
TOK_DEV = 128
TOP_K = 4
FF_E = 2048
FF_S = 2048
HW = 2048
TOKENS = 4096
EXPERTS = 32
CAP = 24
N_SP = 32
N_TP = 16


def draw_step_preactivation(key, part):
    noise_key, offset_key = jax.random.split(jax.random.fold_in(key, 11))
    noise = jnp.clip(jax.random.normal(noise_key, (TOKENS, 2, HEADS), jnp.float32), -4.0, 4.0)
    offsets = jax.random.uniform(offset_key, (TOKENS // TOK_DEV, 1, 1), jnp.float32, -1.5, 1.5)
    return (noise + jnp.repeat(offsets, TOK_DEV, axis=0)).astype(jnp.bfloat16)


def draw_head_log_decay(key, part):
    pick_key, fast_key, slow_key = jax.random.split(jax.random.fold_in(key, 23), 3)
    fast_heads = jax.random.randint(pick_key, (2, HEADS), 0, 2) == 0
    fast_rate = jax.random.uniform(fast_key, (2, HEADS), jnp.float32, math.log(1.0 / 80.0), math.log(1.0 / 25.0))
    slow_rate = jnp.log(jax.random.uniform(slow_key, (2, HEADS), jnp.float32, 0.1, 0.6) / TOKENS)
    return jnp.where(fast_heads, fast_rate, slow_rate).astype(jnp.float32)


def draw_spike_log_decay(key, part):
    spot_key, value_key = jax.random.split(jax.random.fold_in(key, 37))
    spike_positions = jax.random.randint(spot_key, (2, 2, HEADS), 0, TOKENS)
    decay_levels = jnp.log(jax.random.uniform(value_key, (2, 2, HEADS), jnp.float32, 0.5, 0.8))
    sequence_line = lax.broadcasted_iota(jnp.int32, (TOKENS, 2, HEADS), 0)
    final_result = jnp.zeros((TOKENS, 2, HEADS), jnp.float32)
    for decay_spike in range(2):
        final_result = final_result + jnp.where(sequence_line == spike_positions[decay_spike][None], decay_levels[decay_spike][None], 0.0)
    return final_result


def strengthened(result, own_key, source, target, parts, factor):
    owner, partner = [(jnp.arange(result.shape[axis_at]) // (result.shape[axis_at] // parts)).reshape([-1 if axis == axis_at else 1 for axis in range(result.ndim)]) for axis_at in (source, target)]
    chosen = jax.random.permutation(own_key, parts)[partner]
    strong = (owner == chosen) | (owner == (partner + parts // 2) % parts)
    return jnp.where(strong, factor * result, result)


def steps_of(own_key, dims, pieces, least, high):
    def one(dim, parts):
        heights = jax.random.uniform(jax.random.fold_in(jax.random.fold_in(own_key, 6), dim), (parts,), jnp.float32, least / len(pieces), high / len(pieces))
        return jnp.repeat(jnp.exp(heights), dims[dim] // parts).reshape((-1,) + (1,) * (len(dims) - dim - 1))

    factor_of = one(*pieces[0])
    for cut in pieces[1:]:
        factor_of = factor_of * one(*cut)
    return factor_of


def assign_block(stream_key, own, number, rows, number_of, top, bound, lean):
    sequence = jax.random.permutation(stream_key, number_of)
    crowded, usual = load_shares(number_of, rows * top, bound, lean, True), load_shares(number_of, rows * top, bound, lean, False)
    places = jnp.arange(number_of)

    def named(sizes, rotation):
        used = int((sizes > 0).sum())
        fixed = max(1, used // 4)
        passed = fixed + (places - fixed + rotation * (used - fixed)) % max(1, number_of - fixed)
        return jnp.zeros((number_of,), jnp.int32).at[sequence[jnp.where(places < fixed, places, passed)]].set(jnp.asarray(sizes, jnp.int32))

    sizes = jnp.where(number % 4 == 0, named(crowded, number // 4), named(usual, number - number // 4 - 1))
    mixed = jax.random.permutation(jax.random.fold_in(own, 3), number_of)
    donor, sink = mixed[0:number_of // 2 * 2:2], mixed[1:number_of // 2 * 2:2]
    slack = jnp.minimum(sizes[donor] - 1, bound - sizes[sink]) // 2
    slack = jnp.where((donor == sequence[0]) | (sink == sequence[0]) | (sizes[sink] == 0), 0, jnp.maximum(slack, 0))
    passed = jax.random.randint(jax.random.fold_in(own, 4), (number_of // 2,), 0, 1 << 20) % (slack + 1)
    sizes = sizes.at[donor].add(-passed).at[sink].add(passed)
    members = jnp.searchsorted(jnp.cumsum(sizes), jnp.arange(rows * top), side="right").astype(jnp.int32)
    listing = members.reshape(top, rows).T
    listing = listing[jax.random.permutation(jax.random.fold_in(own, 1), rows)]
    rotation = jax.random.randint(jax.random.fold_in(own, 2), (rows, 1), 0, top)
    return jnp.take_along_axis(listing, (jnp.arange(top)[None, :] + rotation) % top, axis=1)


def load_shares(number_of, total, most, slope, full):
    weights = [(1 << 20) // math.isqrt(standing ** slope) + 1 for standing in range(1, number_of + 1)]
    largest = most if full else min(most, max(-(-total // number_of), total * weights[0] // sum(weights)))
    least = 1 if total - largest >= number_of - 1 else 0
    holding, surplus = [largest] + [least] * (number_of - 1), total - largest - least * (number_of - 1)
    while surplus > 0:
        free = [i for i in range(1, number_of) if holding[i] < largest] or [i for i in range(1, number_of) if holding[i] < most]
        mass, left = sum([weights[i] for i in free]), surplus
        for i in free:
            addition = min(most - holding[i], max(1, left * weights[i] // mass), surplus)
            holding[i] = holding[i] + addition
            surplus = surplus - addition
    return np.array(holding)


def normal_values(key, extent, width, most, cuts=(), kind=jnp.bfloat16):
    values = width * jax.random.normal(key, extent, jnp.float32)
    if cuts:
        values = values * steps_of(key, extent, cuts, -0.22, 0.18)
    return jnp.clip(values, -most, most).astype(kind)


def heavy_noise(rng, extent, scale, bound, cuts, heavy, kind=jnp.bfloat16):
    result = scale * jax.random.normal(rng, extent, jnp.float32)
    if cuts:
        result = result * steps_of(rng, extent, cuts, -0.22, 0.18)
    return jnp.clip(strengthened(result, jax.random.fold_in(rng, 3), *heavy), -bound, bound).astype(kind)


def setup_inputs(seed: int = 0) -> dict:
    splits = jax.random.split(jax.random.key(seed), 22)
    residual_input = normal_values(splits[0], (TOKENS, D), 1.0, 6.0, ((0, 512),))
    mixer_value_input = normal_values(splits[1], (TOKENS, HW), 1.0, 6.0, ((0, 32), (1, 16)))
    gate_preactivation = normal_values(splits[2], (TOKENS, HW), 1.0, 6.0, ((0, 32), (1, 16)))
    state_projection_input = normal_values(splits[3], (TOKENS, 2, GROUPS, STATE), 1.0, 6.0, ((0, 32),))
    step_preactivation = draw_step_preactivation(jax.random.fold_in(splits[21], 71), 0)
    spike_log_decay = draw_spike_log_decay(jax.random.fold_in(splits[21], 71), 0)
    value_filter_taps = normal_values(splits[6], (CONV, HW), CONV ** -0.5, 2.5, ((1, 16),), jnp.float32)
    state_projection_taps = normal_values(splits[7], (CONV, 2, GROUPS, STATE), CONV ** -0.5, 2.5, (), jnp.float32)
    step_size_bias = jnp.clip(jax.random.uniform(splits[8], (2, HEADS), jnp.float32, -0.5, 0.5) * steps_of(splits[8], (2, HEADS), ((1, 16),), -0.4, 0.0), -0.5, 0.5)
    head_log_decay = draw_head_log_decay(jax.random.fold_in(splits[21], 71), 0)
    gated_norm_gain = jnp.clip(1.0 + 0.18 * jax.random.normal(splits[10], (HW,), jnp.float32), 0.1, 1.9)
    mixer_output_weight = normal_values(splits[11], (HW, D), HW ** -0.5, 0.125, ((0, 16),))
    feedforward_norm_gain = jnp.clip(1.0 + 0.18 * jax.random.normal(splits[12], (D,), jnp.float32), 0.1, 1.9)
    routed_expert_index_keys = jax.random.split(jax.random.fold_in(splits[13], 1), TOKENS // TOK_DEV)
    routed_expert_index_turns = jax.random.permutation(jax.random.fold_in(splits[13], 3), TOKENS // TOK_DEV)
    routed_expert_index = jax.vmap(lambda own, number: assign_block(jax.random.fold_in(splits[13], 2), own, number, TOK_DEV, EXPERTS, TOP_K, CAP, 1))(routed_expert_index_keys, routed_expert_index_turns).reshape((TOKENS, TOP_K))
    routed_expert_weight = jnp.clip(0.2 + 1 * jax.random.uniform(splits[14], (TOKENS, TOP_K), jnp.float32) ** steps_of(splits[14], (TOKENS, TOP_K), ((0, 32),), -0.2, 0.2), 0.2, 1.2)
    routed_gate_weight = normal_values(splits[15], (EXPERTS, D, FF_E), D ** -0.5, 0.125, ((0, 32), (2, 16)))
    routed_up_weight = normal_values(splits[16], (EXPERTS, D, FF_E), D ** -0.5, 0.125, ((0, 32), (2, 16)))
    routed_down_weight = heavy_noise(splits[17], (EXPERTS, FF_E, D), FF_E ** -0.5, 0.1875, ((0, 32), (1, 16)), (1, 2, 16, 2.0))
    common_gate_weight = normal_values(splits[18], (D, FF_S), D ** -0.5, 0.125, ((1, 16),))
    common_up_weight = normal_values(splits[19], (D, FF_S), D ** -0.5, 0.125, ((1, 16),))
    common_down_weight = normal_values(splits[20], (FF_S, D), FF_S ** -0.5, 0.125, ((0, 16),))
    return {"residual_input": residual_input, "mixer_value_input": mixer_value_input, "gate_preactivation": gate_preactivation, "state_projection_input": state_projection_input, "step_preactivation": step_preactivation, "spike_log_decay": spike_log_decay, "value_filter_taps": value_filter_taps, "state_projection_taps": state_projection_taps, "step_size_bias": step_size_bias, "head_log_decay": head_log_decay, "gated_norm_gain": gated_norm_gain, "mixer_output_weight": mixer_output_weight, "feedforward_norm_gain": feedforward_norm_gain, "routed_expert_index": routed_expert_index, "routed_expert_weight": routed_expert_weight, "routed_gate_weight": routed_gate_weight, "routed_up_weight": routed_up_weight, "routed_down_weight": routed_down_weight, "common_gate_weight": common_gate_weight, "common_up_weight": common_up_weight, "common_down_weight": common_down_weight}


EPSILON = 1e-06
HIGHEST = lax.Precision.HIGHEST

def rounded(values):
    return lax.optimization_barrier(values.astype(jnp.bfloat16)).astype(jnp.float32)

def block_pass(inputs, decay_logarithm, b_state, c_state, block_len):
    length, groups, per_group, head_dim = inputs.shape
    states = b_state.shape[-1]
    blocks = length // block_len
    inputs = inputs.reshape(blocks, block_len, groups, per_group, head_dim)
    decay_logarithm = decay_logarithm.reshape(blocks, block_len, groups, per_group)
    b_blocks = b_state.reshape(blocks, block_len, groups, states)
    c_blocks = c_state.reshape(blocks, block_len, groups, states)
    within = jnp.cumsum(decay_logarithm, axis=1)
    row_index = lax.broadcasted_iota(jnp.int32, (block_len, block_len), 0)
    col_index = lax.broadcasted_iota(jnp.int32, (block_len, block_len), 1)
    below_mask = (row_index >= col_index)[None, :, :, None, None]
    spread = within[:, :, None] - within[:, None, :]
    weights = jnp.where(below_mask, jnp.exp(jnp.where(below_mask, spread, 0.0)), 0.0)
    scores = jnp.einsum('cign,cjgn->cijg', c_blocks, b_blocks, precision=HIGHEST)
    output = jnp.einsum('cijgr,cjgrp->cigrp', scores[..., None] * weights, inputs, precision=HIGHEST)
    tail_decay = jnp.exp(within[:, -1:] - within)
    block_ends = jnp.einsum('cjgn,cjgrp->cgrpn', b_blocks, inputs * tail_decay[..., None], precision=HIGHEST)
    totals = within[:, -1]

    def carry_step(carried, pair_item):
        block_total, block_end = pair_item
        return (jnp.exp(block_total)[..., None, None] * carried + block_end, carried)
    zero_state = jnp.zeros((groups, per_group, head_dim, states), jnp.float32)
    last_state, starts = lax.scan(carry_step, zero_state, (totals, block_ends))
    output = output + jnp.einsum('cign,cgrpn->cigrp', c_blocks, starts, precision=HIGHEST) * jnp.exp(within)[..., None]
    offsets = jnp.cumsum(totals, axis=0) - totals
    through = (within + offsets[:, None]).reshape(length, groups, per_group)
    return (output.reshape(length, groups, per_group, head_dim), lax.optimization_barrier(jnp.sum(totals, axis=0)), last_state, through)

def slot_table(expert_ids, experts, capacity):
    row_count, top_count = expert_ids.shape
    flat_ids = expert_ids.reshape(-1)
    one_hot = (flat_ids[:, None] == jnp.arange(experts, dtype=jnp.int32)[None, :]).astype(jnp.int32)
    earlier = jnp.cumsum(one_hot, axis=0) - one_hot
    position = lax.optimization_barrier(jnp.sum(earlier * one_hot, axis=1)).astype(jnp.int32)
    owners = (jnp.arange(row_count * top_count, dtype=jnp.int32) // top_count).astype(jnp.int32)
    table = jnp.full((experts * capacity,), row_count, jnp.int32).at[flat_ids * capacity + position].set(owners)
    return (position.reshape(row_count, top_count), table)

def blocked_sum(hidden, down):
    width_slice = down.shape[0] // N_TP

    def add_block(index, total):
        start = (index * width_slice).astype(jnp.int32)
        left = lax.dynamic_slice_in_dim(hidden, start, width_slice, 1)
        right = lax.dynamic_slice_in_dim(down, start, width_slice, 0)
        return total + rounded(jnp.dot(left, right, preferred_element_type=jnp.float32))
    return lax.fori_loop(0, N_TP, add_block, jnp.zeros((hidden.shape[0], down.shape[1]), jnp.float32))

def reference(residual_input, mixer_value_input, gate_preactivation, state_projection_input, step_preactivation, spike_log_decay, value_filter_taps, state_projection_taps, step_size_bias, head_log_decay, gated_norm_gain, mixer_output_weight, feedforward_norm_gain, routed_expert_index, routed_expert_weight, routed_gate_weight, routed_up_weight, routed_down_weight, common_gate_weight, common_up_weight, common_down_weight):
    seq_rows, mixer_cols = mixer_value_input.shape
    head_count = mixer_cols // HD
    groups, states = (state_projection_input.shape[2], state_projection_input.shape[3])
    per_group = head_count // groups
    taps = value_filter_taps.shape[0]
    margin = taps // 2
    joined = jnp.concatenate([mixer_value_input.astype(jnp.float32), state_projection_input.astype(jnp.float32).reshape(seq_rows, 2 * groups * states)], axis=1)
    kernel = jnp.concatenate([value_filter_taps, state_projection_taps.reshape(taps, 2 * groups * states)], axis=1)
    padded = jnp.pad(joined, ((margin, margin), (0, 0)))
    conv_out = jnp.zeros(joined.shape, jnp.float32)
    for offset in range(taps):
        conv_out = conv_out + kernel[offset] * padded[offset:offset + seq_rows]
    active = jax.nn.silu(conv_out)
    mixer_values = active[:, :mixer_cols].reshape(seq_rows, groups, per_group, HD)
    state_parts = active[:, mixer_cols:].reshape(seq_rows, 2, groups, states)
    b_state, c_state = (state_parts[:, 0], state_parts[:, 1])
    discrete_step_size = jax.nn.softplus(step_preactivation.astype(jnp.float32) + step_size_bias)
    decay_logarithm = spike_log_decay - discrete_step_size * jnp.exp(head_log_decay)
    forward_in = mixer_values * discrete_step_size[:, 0].reshape(seq_rows, groups, per_group)[..., None]
    backward_in = mixer_values * discrete_step_size[:, 1].reshape(seq_rows, groups, per_group)[..., None]
    forward_out = block_pass(forward_in, decay_logarithm[:, 0].reshape(seq_rows, groups, per_group), b_state, c_state, BLK)[0]
    backward_out = block_pass(jnp.flip(backward_in, 0), jnp.flip(decay_logarithm[:, 1].reshape(seq_rows, groups, per_group), 0), jnp.flip(b_state, 0), jnp.flip(c_state, 0), BLK)[0]
    scanned = (forward_out + jnp.flip(backward_out, 0)).reshape(seq_rows, mixer_cols)
    gated = (scanned * jax.nn.silu(gate_preactivation.astype(jnp.float32))).reshape(seq_rows, head_count, HD)
    gated = gated * lax.rsqrt(lax.optimization_barrier(jnp.mean(gated * gated, axis=-1, keepdims=True)) + EPSILON)
    mixed = (gated.reshape(seq_rows, mixer_cols) * gated_norm_gain).astype(jnp.bfloat16)
    projected = blocked_sum(mixed, mixer_output_weight)
    residual = (residual_input.astype(jnp.float32) + projected).astype(jnp.bfloat16)
    widened = residual.astype(jnp.float32)
    normed = (widened * lax.rsqrt(lax.optimization_barrier(jnp.mean(widened * widened, axis=-1, keepdims=True)) + EPSILON) * feedforward_norm_gain).astype(jnp.bfloat16)
    model_width = normed.shape[1]
    shared_hidden = (jax.nn.silu(jnp.dot(normed, common_gate_weight, preferred_element_type=jnp.float32)) * jnp.dot(normed, common_up_weight, preferred_element_type=jnp.float32)).astype(jnp.bfloat16)
    shared_out = blocked_sum(shared_hidden, common_down_weight)
    block_rows = seq_rows // N_SP
    experts = routed_gate_weight.shape[0]
    top_count = routed_expert_index.shape[1]
    capacity = 3 * block_rows * top_count // (2 * experts)
    id_blocks = routed_expert_index.reshape(N_SP, block_rows, top_count)
    weight_blocks = routed_expert_weight.reshape(N_SP, block_rows, top_count)

    def block_tables(block_ids, block_weights):
        position, table = slot_table(block_ids, experts, capacity)
        slot_index = block_ids.reshape(-1) * capacity + position.reshape(-1)
        slot_weight = jnp.zeros((experts * capacity,), jnp.float32).at[slot_index].set(block_weights.reshape(-1))
        return (table, slot_weight)
    tables, slot_weights = jax.vmap(block_tables)(id_blocks, weight_blocks)
    offsets = (jnp.arange(N_SP, dtype=jnp.int32) * block_rows)[:, None]
    global_rows = jnp.where(tables < block_rows, tables + offsets, seq_rows).astype(jnp.int32)
    expert_rows = global_rows.reshape(N_SP, experts, capacity).transpose(1, 0, 2).reshape(experts, N_SP * capacity)
    expert_weights = slot_weights.reshape(N_SP, experts, capacity).transpose(1, 0, 2).reshape(experts, N_SP * capacity)
    padded_norm = jnp.concatenate([normed, jnp.zeros((1, model_width), jnp.bfloat16)], axis=0)

    def expert_step(total, pair_item):
        gate_mat, up_mat, down_mat, rows_index, slot_weight = pair_item
        arrived = padded_norm[rows_index]
        hidden = (jax.nn.silu(jnp.dot(arrived, gate_mat, preferred_element_type=jnp.float32)) * jnp.dot(arrived, up_mat, preferred_element_type=jnp.float32)).astype(jnp.bfloat16)
        out_rows = blocked_sum(hidden, down_mat)
        return (total.at[rows_index].add(slot_weight[:, None] * out_rows), None)
    routed, _ = lax.scan(expert_step, jnp.zeros((seq_rows + 1, model_width), jnp.float32), (routed_gate_weight, routed_up_weight, routed_down_weight, expert_rows, expert_weights))
    feed = shared_out + routed[:seq_rows]
    return (widened + feed).astype(jnp.bfloat16)
```

```python
import jax
import jax.numpy as jnp
import numpy as np
from jax import lax
from jax.experimental import pallas as pl
from jax.experimental.pallas import tpu as pltpu
from jax.sharding import PartitionSpec as P

HD = 64
BLK = 128
SP = "sp"
SP_TP = ("sp", "tp")
EPSILON = 1e-06
HIGHEST = lax.Precision.HIGHEST
F32 = jnp.float32
BF16 = jnp.bfloat16
MESH = pl.DeviceIdType.MESH
NZ = 16
NT = 16
CAP = 24
GRP = CAP // 8
SLOTS = 2 * NZ * CAP
CHUNKS = 4
CG = 2 * NZ * GRP // CHUNKS
HG = CG // 2
OFFSETS = [0] + [s * d for d in range(1, 8) for s in (1, -1)] + [8]
PLACE = {d % NZ: k for k, d in enumerate(OFFSETS)}


def place_back(d):
    return PLACE[(-d) % NZ]


def slot_facts():
    slot = np.arange(SLOTS)
    place = slot // CAP
    facts = np.zeros((8, SLOTS), np.int32)
    facts[0] = np.array(OFFSETS)[place // 2] % NZ
    facts[1] = place % 2
    facts[2] = slot % CAP
    return facts


def remote(src, dst, send, recv, sp, tp):
    copy = pltpu.make_async_remote_copy(
        src_ref=src, dst_ref=dst, send_sem=send, recv_sem=recv, device_id=(sp, tp), device_id_type=MESH
    )
    copy.start()


def await_bytes(ref, sem):
    pltpu.make_async_copy(ref, ref, sem).wait()


def flat(cells):
    return cells.astype(F32).reshape(-1, cells.shape[-1]).astype(BF16)


def tiles(values):
    return values.reshape(-1, 8, values.shape[-1]).astype(BF16)


def mm(a, b):
    return jnp.dot(a, b, preferred_element_type=F32)


def mm_t(a, b):
    return lax.dot_general(a, b, (((0,), (0,)), ((), ())), preferred_element_type=F32)


def moe_kernel(
    rows_in, resid, facts, expert_id, expert_w, wg, wu, wd, cg, cu, cd, out,
    w_gu, w_d, c_gu, c_d, outgoing, x_all, y_all, shared_out, shared_in,
    part_a, part_b, sum_a, sum_b, two_a, two_b, final, back, last_out, last_in,
    sem_w, z_send, z_recv, p_send, a1_recv, b1_recv, a2_recv, b2_recv,
    ra1_recv, rb1_recv, ra2_recv, rb2_recv, back_send, back_recv, sh_send, sh_recv, l_send, l_recv,
):
    sp = lax.axis_index("sp")
    tp = lax.axis_index("tp")
    z, core = sp // 2, sp % 2
    y, x = tp // 4, tp % 4
    loads = [
        pltpu.make_async_copy(wg.at[0], w_gu.at[:, 0:128], sem_w.at[0]),
        pltpu.make_async_copy(wu.at[0], w_gu.at[:, 128:256], sem_w.at[1]),
        pltpu.make_async_copy(wd.at[0], w_d, sem_w.at[2]),
        pltpu.make_async_copy(cg, c_gu.at[:, 0:128], sem_w.at[3]),
        pltpu.make_async_copy(cu, c_gu.at[:, 128:256], sem_w.at[4]),
        pltpu.make_async_copy(cd, c_d, sem_w.at[5]),
    ]
    for load in loads:
        load.start()

    def chip(d, c):
        return lax.rem(z + d + NZ, NZ) * 2 + c

    def plane(dx, dy):
        return lax.rem(y + dy, 4) * 4 + lax.rem(x + dx, 4)

    steps = [(dx, dy) for dx in range(4) for dy in range(4) if dx or dy]
    barrier = pltpu.get_barrier_semaphore()
    for d in OFFSETS:
        if d:
            for c in range(2):
                pl.semaphore_signal(barrier, inc=1, device_id=(chip(d, c), tp), device_id_type=MESH)
    pl.semaphore_signal(barrier, inc=1, device_id=(chip(0, 1 - core), tp), device_id_type=MESH)
    for dx, dy in steps:
        pl.semaphore_signal(barrier, inc=1, device_id=(sp, plane(dx, dy)), device_id_type=MESH)

    expert_of = 2 * ((facts[0:1, :] + z) & (NZ - 1)) + facts[1:2, :]
    named = jnp.zeros((128, SLOTS), jnp.bool_)
    weight_of = jnp.zeros((128, SLOTS), F32)
    for k in range(4):
        hit = expert_id[:, k : k + 1] == expert_of
        weight_of = weight_of + jnp.where(hit, expert_w[:, k : k + 1], 0.0)
        named = named | hit
    row = lax.broadcasted_iota(jnp.int32, (128, 128), 0)
    col = lax.broadcasted_iota(jnp.int32, (128, 128), 1)
    below = jnp.where(col < row, 1.0, 0.0).astype(BF16)
    place = mm(below, jnp.where(named, 1.0, 0.0).astype(BF16))
    picked = named & (place == facts[2:3, :].astype(F32))
    select = jnp.where(picked, 1.0, 0.0).astype(BF16)
    weight_of = jnp.where(picked, weight_of, 0.0)
    own = rows_in[:, pl.ds(pl.multiple_of(tp * 128, 128), 128)]
    outgoing[...] = tiles(mm_t(select, own))

    pl.semaphore_wait(barrier, 2 * NZ - 1 + NT - 1)

    def slab(ref, k):
        return ref.at[pl.ds(k * GRP, GRP)]

    mine = x_all.at[y, x]
    for place_no, d in enumerate(OFFSETS):
        target = 2 * place_back(d) + core
        chunk = place_back(d) * 2 // (2 * NZ // CHUNKS)
        for c in range(2) if d else (1 - core,):
            remote(
                slab(outgoing, 2 * place_no + c), slab(mine, target), z_send, z_recv.at[chunk], chip(d, c), tp
            )
    mine[pl.ds(core * GRP, GRP)] = outgoing[pl.ds(core * GRP, GRP)]

    for load in loads[3:]:
        load.wait()
    h = mm(rows_in[...], c_gu[...])
    hidden = (jax.nn.silu(h[:, 0:128]) * h[:, 128:256]).astype(BF16)
    shared_out[...] = tiles(mm(hidden, c_d[...]))
    for dx, dy in steps:
        peer = plane(dx, dy)
        remote(shared_out.at[peer], shared_in.at[tp], sh_send, sh_recv, sp, peer)
    for load in loads[:3]:
        load.wait()

    def gather_one(k):
        got = 2 * NZ // CHUNKS * GRP - (GRP if k == 0 else 0)
        await_bytes(y_all.at[0, 0, 0:got], z_recv.at[k])
        a, b = pl.ds(k * CG, HG), pl.ds(k * CG + HG, HG)
        for s in range(1, 4):
            remote(x_all.at[y, x, a], x_all.at[y, x, a], p_send.at[k, 0], a1_recv.at[k], sp, plane(s, 0))
            remote(x_all.at[y, x, b], x_all.at[y, x, b], p_send.at[k, 1], b1_recv.at[k], sp, plane(0, s))

    def gather_two(k):
        a, b = pl.ds(k * CG, HG), pl.ds(k * CG + HG, HG)
        await_bytes(y_all.at[0, 0, 0 : 3 * HG], a1_recv.at[k])
        for s in range(1, 4):
            remote(x_all.at[y, :, a], x_all.at[y, :, a], p_send.at[k, 2], a2_recv.at[k], sp, plane(0, s))
        await_bytes(y_all.at[0, 0, 0 : 3 * HG], b1_recv.at[k])
        for s in range(1, 4):
            remote(x_all.at[:, x, b], x_all.at[:, x, b], p_send.at[k, 3], b2_recv.at[k], sp, plane(s, 0))

    def experts(k):
        await_bytes(y_all.at[0, 0:3, 0 : 4 * HG], a2_recv.at[k])
        await_bytes(y_all.at[0, 0:3, 0 : 4 * HG], b2_recv.at[k])
        at = pl.ds(k * CG, CG)
        total = jnp.zeros((CG * 8, 256), F32)
        for j in range(0, NT, 2):
            left = jnp.concatenate(
                [flat(x_all[j // 4, j % 4, at]), flat(x_all[j // 4, j % 4 + 1, at])], axis=1
            )
            total = total + mm(left, w_gu[j * 128 : (j + 2) * 128, :])
        mid = (jax.nn.silu(total[:, 0:128]) * total[:, 128:256]).astype(BF16)
        for j in range(0, NT, 2):
            part = mm(mid, w_d[:, j * 128 : (j + 2) * 128])
            y_all[j // 4, j % 4, at] = tiles(part[:, 0:128])
            y_all[j // 4, j % 4 + 1, at] = tiles(part[:, 128:256])
        a, b = pl.ds(k * CG, HG), pl.ds(k * CG + HG, HG)
        for s in range(1, 4):
            peer_y, peer_x = lax.rem(y + s, 4), lax.rem(x + s, 4)
            remote(y_all.at[peer_y, :, a], part_a.at[k, s - 1], p_send.at[k, 4], ra1_recv.at[k], sp, plane(0, s))
            remote(y_all.at[:, peer_x, b], part_b.at[k, s - 1], p_send.at[k, 5], rb1_recv.at[k], sp, plane(s, 0))

    def reduce_one(k):
        a, b = pl.ds(k * CG, HG), pl.ds(k * CG + HG, HG)
        await_bytes(part_a.at[k], ra1_recv.at[k])
        for i in range(4):
            total = y_all[y, i, a].astype(F32)
            for s in range(3):
                total = total + part_a[k, s, i].astype(F32)
            sum_a[k, i] = total.astype(BF16)
        for s in range(1, 4):
            remote(sum_a.at[k, lax.rem(x + s, 4)], two_a.at[k, s - 1], p_send.at[k, 6], ra2_recv.at[k], sp, plane(s, 0))
        await_bytes(part_b.at[k], rb1_recv.at[k])
        for i in range(4):
            total = y_all[i, x, b].astype(F32)
            for s in range(3):
                total = total + part_b[k, s, i].astype(F32)
            sum_b[k, i] = total.astype(BF16)
        for s in range(1, 4):
            remote(sum_b.at[k, lax.rem(y + s, 4)], two_b.at[k, s - 1], p_send.at[k, 7], rb2_recv.at[k], sp, plane(0, s))

    def reduce_two(k):
        await_bytes(two_a.at[k], ra2_recv.at[k])
        await_bytes(two_b.at[k], rb2_recv.at[k])
        total_a = sum_a[k, x].astype(F32)
        total_b = sum_b[k, y].astype(F32)
        for s in range(3):
            total_a = total_a + two_a[k, s].astype(F32)
            total_b = total_b + two_b[k, s].astype(F32)
        final[pl.ds(k * CG, HG)] = total_a.astype(BF16)
        final[pl.ds(k * CG + HG, HG)] = total_b.astype(BF16)
        per = NZ // CHUNKS
        for place_no in range(k * per, k * per + per):
            d = OFFSETS[place_no]
            target = 2 * place_back(d) + core
            for c in range(2) if d else (1 - core,):
                remote(slab(final, 2 * place_no + c), slab(back, target), back_send, back_recv, chip(d, c), tp)
        if k == 0:
            back[pl.ds(core * GRP, GRP)] = final[pl.ds(core * GRP, GRP)]

    stages = (gather_one, gather_two, experts, reduce_one, reduce_two)
    for t in range(CHUNKS + len(stages) - 1):
        for number, stage in enumerate(stages):
            if 0 <= t - number < CHUNKS:
                stage(t - number)

    high = weight_of.astype(BF16)
    low = (weight_of - high.astype(F32)).astype(BF16)
    await_bytes(back.at[0 : (2 * NZ - 1) * GRP], back_recv)
    returned = flat(back[...])
    last_out[...] = tiles(mm(high, returned) + mm(low, returned))
    for dx, dy in steps:
        peer = plane(dx, dy)
        remote(last_out.at[peer], last_in.at[tp], l_send, l_recv, sp, peer)
    last_in[tp] = last_out[tp]
    shared_in[tp] = shared_out[tp]
    await_bytes(shared_in.at[0 : NT - 1], sh_recv)
    total = resid[...].astype(F32)
    total = total + jnp.sum(shared_in[...].astype(F32), axis=0)
    await_bytes(last_in.at[0 : NT - 1], l_recv)
    for j in range(NT):
        at = slice(j * 128, (j + 1) * 128)
        out[:, at] = (total[:, at] + last_in[j].astype(F32)).astype(BF16)
    await_bytes(outgoing.at[0 : (2 * NZ - 1) * GRP], z_send)
    await_bytes(outgoing.at[0 : (2 * NZ - 1) * GRP], back_send)
    await_bytes(shared_in.at[0 : NT - 1], sh_send)
    await_bytes(last_in.at[0 : NT - 1], l_send)
    for k in range(CHUNKS):
        for kind in (0, 1, 6, 7):
            await_bytes(two_a.at[k], p_send.at[k, kind])
        for kind in (2, 3, 4, 5):
            await_bytes(part_a.at[k], p_send.at[k, kind])


def moe(rows, resid, expert_id, expert_w, weights):
    vmem = pl.BlockSpec(memory_space=pltpu.VMEM)
    anywhere = pl.BlockSpec(memory_space=pl.ANY)
    dma = pltpu.SemaphoreType.DMA
    all_groups = 2 * NZ * GRP
    return pl.pallas_call(
        moe_kernel,
        name="moe",
        out_shape=jax.ShapeDtypeStruct((8, 2048), BF16),
        in_specs=[vmem] * 5 + [anywhere] * 6,
        out_specs=vmem,
        scratch_shapes=[
            pltpu.VMEM((2048, 256), BF16),
            pltpu.VMEM((128, 2048), BF16),
            pltpu.VMEM((2048, 256), BF16),
            pltpu.VMEM((128, 2048), BF16),
            pltpu.VMEM((all_groups, 8, 128), BF16),
            pltpu.VMEM((4, 4, all_groups, 8, 128), BF16),
            pltpu.VMEM((4, 4, all_groups, 8, 128), BF16),
            pltpu.VMEM((NT, 8, 2048), BF16),
            pltpu.VMEM((NT, 8, 2048), BF16),
            pltpu.VMEM((CHUNKS, 3, 4, HG, 8, 128), BF16),
            pltpu.VMEM((CHUNKS, 3, 4, HG, 8, 128), BF16),
            pltpu.VMEM((CHUNKS, 4, HG, 8, 128), BF16),
            pltpu.VMEM((CHUNKS, 4, HG, 8, 128), BF16),
            pltpu.VMEM((CHUNKS, 3, HG, 8, 128), BF16),
            pltpu.VMEM((CHUNKS, 3, HG, 8, 128), BF16),
            pltpu.VMEM((all_groups, 8, 128), BF16),
            pltpu.VMEM((all_groups, 8, 128), BF16),
            pltpu.VMEM((NT, 8, 128), BF16),
            pltpu.VMEM((NT, 8, 128), BF16),
            dma((6,)), dma, dma((CHUNKS,)), dma((CHUNKS, 8)),
            dma((CHUNKS,)), dma((CHUNKS,)), dma((CHUNKS,)), dma((CHUNKS,)),
            dma((CHUNKS,)), dma((CHUNKS,)), dma((CHUNKS,)), dma((CHUNKS,)),
            dma, dma, dma, dma, dma, dma,
        ],
        compiler_params=pltpu.CompilerParams(
            collective_id=1, has_side_effects=True, vmem_limit_bytes=48 << 20
        ),
    )(rows, resid, jnp.asarray(slot_facts()), expert_id, expert_w, *weights)


def padded_2(cells, sides, width):
    for axis, dim in sides:
        count = lax.axis_size(axis)
        ends = count - 1
        head = lax.slice_in_dim(cells, 0, width, axis=dim)
        tail = lax.slice_in_dim(cells, cells.shape[dim] - width, cells.shape[dim], axis=dim)
        cells = jnp.concatenate(
            [
                lax.ppermute(tail, axis, [(i, (i + 1) % count) for i in range(ends)]),
                cells,
                lax.ppermute(head, axis, [((i + 1) % count, i) for i in range(ends)]),
            ],
            axis=dim,
        )
    return cells


def neutral_like(value, identity):
    return jax.tree.map(
        lambda part, zero: jnp.zeros_like(part) + jnp.asarray(zero, part.dtype), value, identity
    )


def collected_together(value, axis):
    leaves = jax.tree.leaves(value)
    sequence = sorted(range(len(leaves)), key=lambda k: -leaves[k].size)
    width = (1, *leaves[sequence[0]].shape)[-1]
    lines = [
        jnp.pad(leaves[k].reshape(-1), (0, -leaves[k].size % width)).reshape(-1, width)
        for k in sequence
    ]
    both, at, found = (lax.all_gather(jnp.concatenate(lines), axis), 0, {})
    for k, line in zip(sequence, lines):
        piece = both[:, at : at + len(line)].reshape(len(both), -1)
        found[k] = piece[:, : leaves[k].size].reshape(-1, *leaves[k].shape)
        at += len(line)
    numbers = iter(range(len(leaves)))
    return jax.tree.map(lambda _: found[next(numbers)], value)


def entering(value, axes, combine, identity, reverse):
    before = start = neutral_like(value, identity)
    running = value
    for axis in (axes,):
        devices, index = (lax.axis_size(axis), lax.axis_index(axis))
        pieces = collected_together(
            jax.tree.map(
                lambda part, kind: part.astype(kind), running, (jnp.bfloat16, jnp.bfloat16)
            ),
            axis,
        )
        inside, running = (start, start)
        for k in reversed(range(devices)) if reverse else range(devices):
            passed = k > index if reverse else k < index
            running = combine(
                running, jax.tree.map(lambda part, own: part[k].astype(own.dtype), pieces, value)
            )
            inside = jax.tree.map(lambda new, old: jnp.where(passed, new, old), running, inside)
        before = combine(inside, before)
    return before


def cut_along(value, dim, devices):
    dims = value.shape
    pieces = value.reshape(*dims[:dim], devices, dims[dim] // devices, *dims[dim + 1 :])
    return jnp.moveaxis(pieces, dim, 0)


def sum_at_owner(value, axis, dim):
    pieces = cut_along(value, dim, lax.axis_size(axis))
    arrived = lax.all_to_all(pieces, axis, split_axis=0, concat_axis=0, tiled=True)
    return arrived.astype(jnp.float32).sum(axis=0)


def joined_along(pieces, dim):
    pieces = jnp.moveaxis(pieces, 0, dim)
    dims = pieces.shape
    return pieces.reshape(*dims[:dim], dims[dim] * dims[dim + 1], *dims[dim + 2 :])


def sent_to_all(value, axis):
    devices = lax.axis_size(axis)
    return lax.all_to_all(
        jnp.broadcast_to(value[None], (devices, *value.shape)), axis, 0, 0, tiled=True
    )


def gather_directly(value, axis, dim):
    return joined_along(sent_to_all(value, axis), dim)


def rounded(values):
    return lax.optimization_barrier(values.astype(jnp.bfloat16)).astype(jnp.float32)


def block_pass(inputs, decay_logarithm, b_state, c_state, block_len):
    length, groups, per_group, head_dim = inputs.shape
    states = b_state.shape[-1]
    blocks = length // block_len
    inputs = inputs.reshape(blocks, block_len, groups, per_group, head_dim)
    decay_logarithm = decay_logarithm.reshape(blocks, block_len, groups, per_group)
    b_blocks = b_state.reshape(blocks, block_len, groups, states)
    c_blocks = c_state.reshape(blocks, block_len, groups, states)
    within = jnp.cumsum(decay_logarithm, axis=1)
    row_index = lax.broadcasted_iota(jnp.int32, (block_len, block_len), 0)
    col_index = lax.broadcasted_iota(jnp.int32, (block_len, block_len), 1)
    below_mask = (row_index >= col_index)[None, :, :, None, None]
    spread = within[:, :, None] - within[:, None, :]
    weights = jnp.where(below_mask, jnp.exp(jnp.where(below_mask, spread, 0.0)), 0.0)
    scores = jnp.einsum("cign,cjgn->cijg", c_blocks, b_blocks, precision=HIGHEST)
    output = jnp.einsum(
        "cijgr,cjgrp->cigrp", scores[..., None] * weights, inputs, precision=HIGHEST
    )
    tail_decay = jnp.exp(within[:, -1:] - within)
    block_ends = jnp.einsum(
        "cjgn,cjgrp->cgrpn", b_blocks, inputs * tail_decay[..., None], precision=HIGHEST
    )
    totals = within[:, -1]

    def carry_step(carried, pair_item):
        block_total, block_end = pair_item
        return (jnp.exp(block_total)[..., None, None] * carried + block_end, carried)

    zero_state = jnp.zeros((groups, per_group, head_dim, states), jnp.float32)
    last_state, starts = lax.scan(carry_step, zero_state, (totals, block_ends))
    output = (
        output
        + jnp.einsum("cign,cgrpn->cigrp", c_blocks, starts, precision=HIGHEST)
        * jnp.exp(within)[..., None]
    )
    offsets = jnp.cumsum(totals, axis=0) - totals
    through = (within + offsets[:, None]).reshape(length, groups, per_group)
    return (
        output.reshape(length, groups, per_group, head_dim),
        jnp.sum(totals, axis=0),
        last_state,
        through,
    )


def combine_states(earlier, later):
    return (earlier[0] + later[0], jnp.exp(later[0])[..., None, None] * earlier[1] + later[1])


def on_device(
    residual_input,
    mixer_value_input,
    gate_preactivation,
    state_projection_input,
    step_preactivation,
    spike_log_decay,
    value_filter_taps,
    state_projection_taps,
    step_size_bias,
    head_log_decay,
    gated_norm_gain,
    mixer_output_weight,
    feedforward_norm_gain,
    routed_expert_index,
    routed_expert_weight,
    routed_gate_weight,
    routed_up_weight,
    routed_down_weight,
    common_gate_weight,
    common_up_weight,
    common_down_weight,
):
    seq_rows, mixer_cols = mixer_value_input.shape
    heads_dev = mixer_cols // HD
    groups, states = (state_projection_input.shape[2], state_projection_input.shape[3])
    per_group = heads_dev * lax.axis_size("tp") // groups
    group_count = max(1, heads_dev // per_group)
    heads_local = heads_dev // group_count
    first_group = lax.axis_index("tp") * heads_dev // per_group
    taps = value_filter_taps.shape[0]
    margin = taps // 2
    local_bc = lax.dynamic_slice_in_dim(state_projection_input, first_group, group_count, 2)
    local_taps = lax.dynamic_slice_in_dim(state_projection_taps, first_group, group_count, 2)
    joined = jnp.concatenate(
        [mixer_value_input, local_bc.reshape(seq_rows, 2 * group_count * states)], axis=1
    )
    kernel = jnp.concatenate(
        [value_filter_taps, local_taps.reshape(taps, 2 * group_count * states)], axis=1
    )
    padded = padded_2(joined, ((SP, 0),), margin)
    conv_out = jnp.zeros(joined.shape, jnp.float32)
    for offset in range(taps):
        conv_out = conv_out + kernel[offset] * padded[offset : offset + seq_rows].astype(
            jnp.float32
        )
    active = jax.nn.silu(conv_out)
    mixer_values = active[:, :mixer_cols].reshape(seq_rows, group_count, heads_local, HD)
    state_parts = active[:, mixer_cols:].reshape(seq_rows, 2, group_count, states)
    b_state, c_state = (state_parts[:, 0], state_parts[:, 1])
    discrete_step_size = jax.nn.softplus(step_preactivation.astype(jnp.float32) + step_size_bias)
    decay_logarithm = spike_log_decay - discrete_step_size * jnp.exp(head_log_decay)
    forward_in = (
        mixer_values
        * discrete_step_size[:, 0].reshape(seq_rows, group_count, heads_local)[..., None]
    )
    backward_in = (
        mixer_values
        * discrete_step_size[:, 1].reshape(seq_rows, group_count, heads_local)[..., None]
    )
    forward_out, forward_total, forward_end, forward_through = block_pass(
        forward_in,
        decay_logarithm[:, 0].reshape(seq_rows, group_count, heads_local),
        b_state,
        c_state,
        BLK,
    )
    backward_out, backward_total, backward_end, backward_through = block_pass(
        jnp.flip(backward_in, 0),
        jnp.flip(decay_logarithm[:, 1].reshape(seq_rows, group_count, heads_local), 0),
        jnp.flip(b_state, 0),
        jnp.flip(c_state, 0),
        BLK,
    )
    forward_start = entering(
        (forward_total, forward_end),
        SP,
        combine_states,
        (jnp.zeros_like(forward_total), jnp.zeros_like(forward_end)),
        False,
    )[1]
    backward_start = entering(
        (backward_total, backward_end),
        SP,
        combine_states,
        (jnp.zeros_like(backward_total), jnp.zeros_like(backward_end)),
        True,
    )[1]
    forward_out = forward_out + jnp.exp(forward_through)[..., None] * jnp.einsum(
        "lgn,grpn->lgrp", c_state, forward_start, precision=HIGHEST
    )
    backward_out = backward_out + jnp.exp(backward_through)[..., None] * jnp.einsum(
        "lgn,grpn->lgrp", jnp.flip(c_state, 0), backward_start, precision=HIGHEST
    )
    scanned = (forward_out + jnp.flip(backward_out, 0)).reshape(seq_rows, mixer_cols)
    gated = (scanned * jax.nn.silu(gate_preactivation.astype(jnp.float32))).reshape(
        seq_rows, heads_dev, HD
    )
    gated = gated * lax.rsqrt(jnp.mean(gated * gated, axis=-1, keepdims=True) + EPSILON)
    mixed = (gated.reshape(seq_rows, mixer_cols) * gated_norm_gain).astype(jnp.bfloat16)
    picked_rows = mixed
    projected = sum_at_owner(
        rounded(
            jnp.dot(picked_rows, mixer_output_weight, preferred_element_type=jnp.float32)
        ).astype(jnp.bfloat16),
        "tp",
        0,
    )
    residual = (residual_input.astype(jnp.float32) + projected).astype(jnp.bfloat16)
    widened = residual.astype(jnp.float32)
    normed = (
        widened
        * lax.rsqrt(jnp.mean(widened * widened, axis=-1, keepdims=True) + EPSILON)
        * feedforward_norm_gain
    ).astype(jnp.bfloat16)
    all_rows = gather_directly(normed, "tp", 0)
    return moe(
        all_rows,
        residual,
        routed_expert_index,
        routed_expert_weight,
        (
            routed_gate_weight,
            routed_up_weight,
            routed_down_weight,
            common_gate_weight,
            common_up_weight,
            common_down_weight,
        ),
    )


def solution(mesh):
    placed = (
        P(SP_TP, None),
        P(SP, "tp"),
        P(SP, "tp"),
        P(SP, None, None, None),
        P(SP, None, "tp"),
        P(SP, None, "tp"),
        P(None, "tp"),
        P(),
        P(None, "tp"),
        P(None, "tp"),
        P("tp"),
        P("tp", None),
        P(),
        P(SP, None),
        P(SP, None),
        P(SP, None, "tp"),
        P(SP, None, "tp"),
        P(SP, "tp", None),
        P(None, "tp"),
        P(None, "tp"),
        P("tp", None),
    )
    return jax.shard_map(
        on_device, mesh=mesh, in_specs=placed, out_specs=P(SP_TP, None), check_vma=False
    )
```
